32 devices in a mesh: fs: 8 (over z, y), tp: 4 (over x, core).
Axes of the slice: x: 2, y: 2, z: 4, core: 2. Of those that a mesh axis runs over, the one named last changes fastest.
Arguments:
- resid: bfloat16 [12288, 2048], P(('fs', 'tp')), may hold values from -6 to 6
- norm1_gain: float32 [2048], replicated, may hold values from 0.1 to 1.9
- w_value: float32 [2048, 2048], P('fs', 'tp'), may hold values from -0.125 to 0.125
- w_gate: float32 [2048, 2048], P('fs', 'tp'), may hold values from -0.125 to 0.125
- value_scale: float32 [2048], replicated, may hold values from 0.3 to 3
- gate_scale: float32 [2048], replicated, may hold values from 0.5 to 3
- conv_taps: float32 [31, 2048], replicated, may hold values from -1 to 1
- conv_gain: float32 [2048], replicated, may hold values from 0.1 to 1.9
- w_point: float32 [2048, 2048], P('tp', 'fs'), may hold values from -0.125 to 0.125
- point_scale: float32 [2048], P('fs'), may hold values from 0.5 to 3
- norm2_gain: float32 [2048], replicated, may hold values from 0.1 to 1.9
- w_up: float32 [2048, 8192], P('fs', 'tp'), may hold values from -0.125 to 0.125
- up_scale: float32 [8192], P('tp'), may hold values from 0.5 to 1.5
- w_down: float32 [8192, 2048], P('tp', 'fs'), may hold values from -0.0625 to 0.0625
- down_scale: float32 [2048], P('fs'), may hold values from 0.3 to 1
Outputs:
- layer_out: bfloat16 [12288, 2048], P(('fs', 'tp'))
The draws below stay inside these ranges and needn't reach their ends.
All inputs are finite; a program needn't handle non-finite values.
Results may differ from the reference program's by a relative error of at most 0.015.
Values may be sent and summed in bfloat16 or wider, within the bound.
A program may use at most 128 MiB of HBM per device.

```python
import math
import jax
import jax.numpy as jnp
from jax import lax

D = 2048
CH = 2048
FF = 8192
KERNEL = 31
GROUPS = 4
LEN = 1536
TOKENS = 12288
N_TP = 4


def levels(stream_key, extent, shards, low, top_value):
    level = 1.0
    for position, shards_of in shards:
        heights = jax.random.uniform(jax.random.fold_in(jax.random.fold_in(stream_key, 6), position), (shards_of,), jnp.float32, low / len(shards), top_value / len(shards))
        level = level * jnp.repeat(jnp.exp(heights), extent[position] // shards_of).reshape((-1,) + (1,) * (len(extent) - 1 - position))
    return level


def noise(own_key, extent, scale, most, pieces=(), kind=jnp.bfloat16):
    entries = scale * jax.random.normal(own_key, extent, jnp.float32)
    if pieces:
        entries = entries * levels(own_key, extent, pieces, -0.22, 0.18)
    return jnp.clip(entries, -most, most).astype(kind)


def setup_inputs(seed: int = 0) -> dict:
    key_list = jax.random.split(jax.random.key(seed), 16)
    return {
        "resid": noise(key_list[0], (TOKENS, D), 1.0, 6.0, ((0, 32),)),
        "norm1_gain": jnp.clip(1.0 + 0.18 * jax.random.normal(key_list[1], (D,), jnp.float32), 0.1, 1.9),
        "w_value": noise(key_list[2], (D, CH), D ** -0.5, 0.125, ((0, 8), (1, 4)), jnp.float32),
        "w_gate": noise(key_list[3], (D, CH), D ** -0.5, 0.125, ((0, 8), (1, 4)), jnp.float32),
        "value_scale": jnp.clip(jnp.exp(jax.random.uniform(key_list[4], (CH,), jnp.float32, math.log(0.3), math.log(3.0))), 0.3, 3.0),
        "gate_scale": jnp.clip(jnp.exp(jax.random.uniform(key_list[5], (CH,), jnp.float32, math.log(0.5), math.log(3.0))), 0.5, 3.0),
        "conv_taps": noise(key_list[6], (KERNEL, CH), KERNEL ** -0.5, 1.0, (), jnp.float32),
        "conv_gain": jnp.clip(1.0 + 0.18 * jax.random.normal(key_list[7], (CH,), jnp.float32), 0.1, 1.9),
        "w_point": noise(key_list[8], (CH, D), CH ** -0.5, 0.125, ((0, 4), (1, 8)), jnp.float32),
        "point_scale": jnp.clip(jnp.exp(math.log(3.0) - 1.7917595 * jax.random.uniform(key_list[9], (D,), jnp.float32) ** levels(key_list[9], (D,), ((0, 8),), -0.2, 0.2)), 0.5, 3.0),
        "norm2_gain": jnp.clip(1.0 + 0.18 * jax.random.normal(key_list[10], (D,), jnp.float32), 0.1, 1.9),
        "w_up": noise(key_list[11], (D, FF), D ** -0.5, 0.125, ((0, 8), (1, 4)), jnp.float32),
        "up_scale": jnp.clip(jnp.exp(math.log(1.5) - 1.0986123 * jax.random.uniform(key_list[12], (FF,), jnp.float32) ** levels(key_list[12], (FF,), ((0, 4),), -0.2, 0.2)), 0.5, 1.5),
        "w_down": noise(key_list[13], (FF, D), FF ** -0.5, 0.0625, ((0, 4), (1, 8)), jnp.float32),
        "down_scale": jnp.clip(jnp.exp(math.log(1.0) - 1.2039728 * jax.random.uniform(key_list[14], (D,), jnp.float32) ** levels(key_list[14], (D,), ((0, 8),), -0.2, 0.2)), 0.3, 1.0),
    }


def rms_scaled(values, gain):
    data = values.astype(jnp.float32)
    return data * lax.rsqrt(lax.optimization_barrier(jnp.mean(data * data, axis=-1, keepdims=True)) + 1e-06) * gain

def reference(resid, norm1_gain, w_value, w_gate, value_scale, gate_scale, conv_taps, conv_gain, w_point, point_scale, norm2_gain, w_up, up_scale, w_down, down_scale):
    value_bf = w_value.astype(jnp.bfloat16)
    gate_bf = w_gate.astype(jnp.bfloat16)
    point_bf = w_point.astype(jnp.bfloat16)
    up_bf = w_up.astype(jnp.bfloat16)
    down_bf = w_down.astype(jnp.bfloat16)
    normed = rms_scaled(resid, norm1_gain).astype(jnp.bfloat16)
    value = jnp.dot(normed, value_bf, preferred_element_type=jnp.float32) * value_scale
    gate = jnp.dot(normed, gate_bf, preferred_element_type=jnp.float32) * gate_scale
    glu = (value * jax.nn.sigmoid(gate)).astype(jnp.bfloat16)
    reach = KERNEL // 2
    seqs = glu.reshape(-1, LEN, CH).astype(jnp.float32)
    padded = jnp.pad(seqs, ((0, 0), (reach, reach), (0, 0)))
    conv = jnp.zeros(seqs.shape, jnp.float32)
    for offset in range(KERNEL):
        conv = conv + conv_taps[offset] * padded[:, offset:offset + LEN]
    grouped = conv.reshape(-1, CH // GROUPS, GROUPS)
    gmean = lax.optimization_barrier(jnp.mean(grouped, axis=-2, keepdims=True))
    gsquare = lax.optimization_barrier(jnp.mean(grouped * grouped, axis=-2, keepdims=True))
    scaled = ((grouped - gmean) * lax.rsqrt(gsquare - gmean * gmean + 1e-05)).reshape(-1, CH) * conv_gain
    act = jax.nn.silu(scaled).astype(jnp.bfloat16)
    mixed = jnp.dot(act, point_bf, preferred_element_type=jnp.float32) * point_scale
    middle = (resid.astype(jnp.float32) + mixed).astype(jnp.bfloat16)
    normed2 = rms_scaled(middle, norm2_gain).astype(jnp.bfloat16)
    upper = jnp.dot(normed2, up_bf, preferred_element_type=jnp.float32) * up_scale
    hidden = jnp.square(jax.nn.relu(upper)).astype(jnp.bfloat16)
    block = FF // N_TP
    hid_blocks = jnp.transpose(hidden.reshape(hidden.shape[0], N_TP, block), (1, 0, 2))
    down_blocks = down_bf.reshape(N_TP, block, D)

    def add_block(total, pair):
        hid_block, down_block = pair
        partial_value = (jnp.dot(hid_block, down_block, preferred_element_type=jnp.float32) * down_scale).astype(jnp.bfloat16)
        partial_value = lax.optimization_barrier(partial_value)
        return (total + partial_value.astype(jnp.float32), None)
    total, _ = lax.scan(add_block, jnp.zeros((hidden.shape[0], D), jnp.float32), (hid_blocks, down_blocks))
    return (middle.astype(jnp.float32) + total).astype(jnp.bfloat16)
```

```python
import functools

import jax
import jax.numpy as jnp
from jax import lax
from jax.experimental import pallas as pl
from jax.experimental.pallas import tpu as pltpu
from jax.sharding import PartitionSpec as P


GROUPS = 4
CORES = 2
MESH = pl.DeviceIdType.MESH


def rms_scaled(values, gain):
    data = values.astype(jnp.float32)
    return data * lax.rsqrt(jnp.mean(data * data, axis=-1, keepdims=True) + 1e-06) * gain


def depthwise(padded, taps, length):
    wide = padded.astype(jnp.float32)
    conv = jnp.zeros((length, wide.shape[1]), jnp.float32)
    for offset in range(taps.shape[0]):
        conv = conv + taps[offset] * wide[offset : offset + length]
    return conv


def place(n):
    me = lax.axis_index("tp")
    core = lax.rem(me, CORES)
    chip = me // CORES
    chips = n // CORES
    partner = chip * CORES + (CORES - 1 - core)
    return me, core, chip, chips, partner


def chip_core(chip, core, chips):
    return lax.rem(chip + 2 * chips, chips) * CORES + core


def greet(core, chip, chips, partner):
    barrier = pltpu.get_barrier_semaphore()
    pl.semaphore_signal(barrier, inc=1, device_id={"tp": partner}, device_id_type=MESH)
    for d in range(1, chips):
        pl.semaphore_signal(
            barrier, inc=1, device_id={"tp": chip_core(chip + d, core, chips)}, device_id_type=MESH
        )
    pl.semaphore_wait(barrier, chips)


def gather_kernel(n, pieces, x_ref, out_ref, own_sem, far_send, far_recv, near_send, near_recv):
    me, core, chip, chips, partner = place(n)
    rows = x_ref.shape[0]
    step = rows // pieces
    greet(core, chip, chips, partner)

    def spot(owner, k):
        return out_ref.at[pl.ds(pl.multiple_of(owner * rows + k * step, step), step)]

    def src(k):
        return x_ref.at[pl.ds(k * step, step)]

    def far(d, k, owner, target):
        return pltpu.make_async_remote_copy(
            src_ref=src(k), dst_ref=spot(owner, k), send_sem=far_send.at[d - 1, k],
            recv_sem=far_recv.at[d - 1, k], device_id={"tp": target}, device_id_type=MESH)

    def near(d, k, owner, own):
        return pltpu.make_async_remote_copy(
            src_ref=src(k) if own else spot(owner, k), dst_ref=spot(owner, k),
            send_sem=near_send.at[d, k], recv_sem=near_recv.at[d, k],
            device_id={"tp": partner}, device_id_type=MESH)

    for k in range(pieces):
        for d in range(1, chips):
            far(d, k, me, chip_core(chip + d, core, chips)).start()
    for k in range(pieces):
        near(0, k, me, True).start()
    own = pltpu.make_async_copy(x_ref, out_ref.at[pl.ds(pl.multiple_of(me * rows, rows), rows)], own_sem)
    own.start()
    for k in range(pieces):
        for d in range(1, chips):
            owner = chip_core(chip - d, core, chips)
            far(d, k, owner, partner).wait_recv()
            near(d, k, owner, False).start()
    own.wait()
    for k in range(pieces):
        for d in range(1, chips):
            far(d, k, me, chip_core(chip + d, core, chips)).wait_send()
        for d in range(chips):
            sent = chip_core(chip - d, core, chips)
            got = chip_core(chip - d, CORES - 1 - core, chips)
            near(d, k, sent, d == 0).wait_send()
            near(d, k, got, d == 0).wait_recv()


def tp_gather(x, n, cid):
    rows, width = x.shape
    chips = n // CORES
    pieces = 4
    sent = 2 * rows * width * (n - 1)
    return pl.pallas_call(
        functools.partial(gather_kernel, n, pieces),
        out_shape=jax.ShapeDtypeStruct((rows * n, width), x.dtype),
        in_specs=[pl.BlockSpec(memory_space=pltpu.VMEM)],
        out_specs=pl.BlockSpec(memory_space=pl.ANY),
        scratch_shapes=[
            pltpu.SemaphoreType.DMA,
            pltpu.SemaphoreType.DMA((chips - 1, pieces)),
            pltpu.SemaphoreType.DMA((chips - 1, pieces)),
            pltpu.SemaphoreType.DMA((chips, pieces)),
            pltpu.SemaphoreType.DMA((chips, pieces)),
        ],
        compiler_params=pltpu.CompilerParams(collective_id=cid, has_side_effects=True),
        cost_estimate=pl.CostEstimate(flops=200_000_000, bytes_accessed=sent, transcendentals=0),
        name="tp_gather",
    )(x)


def scatter_kernel(n, pieces, p_ref, near_ref, far_ref, mine, theirs, load_sem, near_send, near_recv, far_send, far_recv):
    _, core, chip, chips, partner = place(n)
    rows = near_ref.shape[0]
    step = rows // pieces
    other = CORES - 1 - core
    greet(core, chip, chips, partner)

    def part(owner, k):
        return p_ref.at[pl.ds(pl.multiple_of(owner * rows + k * step, step), step)]

    def near(d, k):
        dst = near_ref.at[pl.ds(k * step, step)] if d == 0 else theirs.at[d - 1, pl.ds(k * step, step)]
        return pltpu.make_async_remote_copy(
            src_ref=part(chip_core(chip + d, other, chips), k), dst_ref=dst,
            send_sem=near_send.at[d, k], recv_sem=near_recv.at[d, k],
            device_id={"tp": partner}, device_id_type=MESH)

    def load(d, k):
        return pltpu.make_async_copy(
            part(chip_core(chip + d, core, chips), k), mine.at[d - 1, pl.ds(k * step, step)], load_sem.at[d - 1, k])

    def far(d, k):
        return pltpu.make_async_remote_copy(
            src_ref=mine.at[d - 1, pl.ds(k * step, step)], dst_ref=far_ref.at[d - 1, pl.ds(k * step, step)],
            send_sem=far_send.at[d - 1, k], recv_sem=far_recv.at[d - 1, k],
            device_id={"tp": chip_core(chip + d, core, chips)}, device_id_type=MESH)

    for k in range(pieces):
        for d in range(1, chips):
            near(d, k).start()
            load(d, k).start()
    for k in range(pieces):
        near(0, k).start()
    for k in range(pieces):
        for d in range(1, chips):
            near(d, k).wait_recv()
            load(d, k).wait()
            at = pl.ds(k * step, step)
            total = mine[d - 1, at].astype(jnp.float32) + theirs[d - 1, at].astype(jnp.float32)
            mine[d - 1, at] = total.astype(mine.dtype)
            far(d, k).start()
    for k in range(pieces):
        near(0, k).wait_recv()
        for d in range(chips):
            near(d, k).wait_send()
        for d in range(1, chips):
            far(d, k).wait()


def tp_scatter(part, n, cid):
    rows, width = part.shape[0] // n, part.shape[1]
    chips = n // CORES
    pieces = 4
    sent = 2 * rows * width * (n - 1)
    return pl.pallas_call(
        functools.partial(scatter_kernel, n, pieces),
        out_shape=(
            jax.ShapeDtypeStruct((rows, width), part.dtype),
            jax.ShapeDtypeStruct((chips - 1, rows, width), part.dtype),
        ),
        in_specs=[pl.BlockSpec(memory_space=pl.ANY)],
        out_specs=(pl.BlockSpec(memory_space=pl.ANY), pl.BlockSpec(memory_space=pl.ANY)),
        scratch_shapes=[
            pltpu.VMEM((chips - 1, rows, width), part.dtype),
            pltpu.VMEM((chips - 1, rows, width), part.dtype),
            pltpu.SemaphoreType.DMA((chips - 1, pieces)),
            pltpu.SemaphoreType.DMA((chips, pieces)),
            pltpu.SemaphoreType.DMA((chips, pieces)),
            pltpu.SemaphoreType.DMA((chips - 1, pieces)),
            pltpu.SemaphoreType.DMA((chips - 1, pieces)),
        ],
        compiler_params=pltpu.CompilerParams(collective_id=cid, has_side_effects=True),
        cost_estimate=pl.CostEstimate(flops=200_000_000, bytes_accessed=sent, transcendentals=0),
        name="tp_scatter",
    )(part)


def scattered_sum(part, n, rank, cid):
    rows = part.shape[0] // n
    near, far = tp_scatter(part, n, cid)
    own = lax.dynamic_slice_in_dim(part, rank * rows, rows, 0)
    total = own.astype(jnp.float32) + near.astype(jnp.float32)
    for d in range(far.shape[0]):
        total = total + far[d].astype(jnp.float32)
    return total


def stats_kernel(n, x_ref, out_ref, recv, send_sem, recv_sem):
    me = lax.axis_index("tp")
    barrier = pltpu.get_barrier_semaphore()
    for d in range(1, n):
        pl.semaphore_signal(barrier, inc=1, device_id={"tp": lax.rem(me + d, n)}, device_id_type=MESH)
    pl.semaphore_wait(barrier, n - 1)

    def send(d):
        return pltpu.make_async_remote_copy(
            src_ref=x_ref, dst_ref=recv.at[d - 1], send_sem=send_sem.at[d - 1],
            recv_sem=recv_sem.at[d - 1], device_id={"tp": lax.rem(me + d, n)}, device_id_type=MESH)

    for d in range(1, n):
        send(d).start()
    total = x_ref[...]
    for d in range(1, n):
        send(d).wait_recv()
        total = total + recv[d - 1]
    out_ref[...] = total
    for d in range(1, n):
        send(d).wait_send()


def tp_sum(x, n, cid):
    return pl.pallas_call(
        functools.partial(stats_kernel, n),
        out_shape=jax.ShapeDtypeStruct(x.shape, x.dtype),
        in_specs=[pl.BlockSpec(memory_space=pltpu.VMEM)],
        out_specs=pl.BlockSpec(memory_space=pltpu.VMEM),
        scratch_shapes=[
            pltpu.VMEM((n - 1,) + x.shape, x.dtype),
            pltpu.SemaphoreType.DMA((n - 1,)),
            pltpu.SemaphoreType.DMA((n - 1,)),
        ],
        compiler_params=pltpu.CompilerParams(collective_id=cid, has_side_effects=True),
        cost_estimate=pl.CostEstimate(flops=20_000_000, bytes_accessed=4 * x.size * n, transcendentals=0),
        name="tp_sum",
    )(x)


def shards(
    resid,
    norm1_gain,
    w_value,
    w_gate,
    value_scale,
    gate_scale,
    conv_taps,
    conv_gain,
    w_point,
    point_scale,
    norm2_gain,
    w_up,
    up_scale,
    w_down,
    down_scale,
):
    tok_rows = resid.shape[0]
    n = lax.axis_size("tp")
    rank = lax.axis_index("tp")
    seq_len = tok_rows * n
    channels = value_scale.shape[0]
    group_width = channels // GROUPS
    reach = conv_taps.shape[0] // 2
    own_width = w_value.shape[1]
    first_bf = jnp.concatenate(
        [w_value.astype(jnp.bfloat16), w_gate.astype(jnp.bfloat16), (w_point * point_scale).T.astype(jnp.bfloat16)],
        axis=1,
    )
    first_rows = lax.all_gather(first_bf, "fs", axis=0, tiled=True)
    up_cols = lax.all_gather(w_up.astype(jnp.bfloat16), "fs", axis=0, tiled=True)
    down_part = lax.all_gather((w_down * down_scale).astype(jnp.bfloat16), "fs", axis=1, tiled=True)
    first = rank * own_width
    own_value_scale = lax.dynamic_slice_in_dim(value_scale, first, own_width, 0)
    own_gate_scale = lax.dynamic_slice_in_dim(gate_scale, first, own_width, 0)
    own_taps = lax.dynamic_slice_in_dim(conv_taps, first, own_width, 1)
    own_gain = lax.dynamic_slice_in_dim(conv_gain, first, own_width, 0)
    normed = rms_scaled(resid, norm1_gain).astype(jnp.bfloat16)
    piece = tp_gather(normed, n, 1)
    value = jnp.dot(piece, first_rows[:, :own_width], preferred_element_type=jnp.float32) * own_value_scale
    gate = (
        jnp.dot(piece, first_rows[:, own_width : 2 * own_width], preferred_element_type=jnp.float32)
        * own_gate_scale
    )
    glu_seq = (value * jax.nn.sigmoid(gate)).astype(jnp.bfloat16)
    padded = jnp.pad(glu_seq, ((reach, reach), (0, 0)))
    conv = depthwise(padded, own_taps, seq_len)
    member = ((first + jnp.arange(own_width)) % GROUPS)[None, :] == jnp.arange(GROUPS)[:, None]
    member = member.astype(jnp.float32)
    flip = (((1,), (1,)), ((), ()))
    sums = lax.dot_general(member, conv, flip, precision=lax.Precision.HIGHEST)
    squares = lax.dot_general(member, conv * conv, flip, precision=lax.Precision.HIGHEST)
    totals = tp_sum(jnp.concatenate([sums, squares], axis=0), n, 2)
    spread = (((0,), (0,)), ((), ()))
    gmean = lax.dot_general(totals[:GROUPS] / group_width, member, spread, precision=lax.Precision.HIGHEST)
    gsquare = lax.dot_general(totals[GROUPS:] / group_width, member, spread, precision=lax.Precision.HIGHEST)
    scaled = (conv - gmean) * lax.rsqrt(gsquare - gmean * gmean + 1e-05) * own_gain
    act = jax.nn.silu(scaled).astype(jnp.bfloat16)
    mixed_part = lax.dot_general(
        act, first_rows[:, 2 * own_width :], flip, preferred_element_type=jnp.float32
    ).astype(jnp.bfloat16)
    mixed = scattered_sum(mixed_part, n, rank, 3)
    middle = (resid.astype(jnp.float32) + mixed).astype(jnp.bfloat16)
    normed2 = rms_scaled(middle, norm2_gain).astype(jnp.bfloat16)
    tokens = tp_gather(normed2, n, 4)
    upper = jnp.dot(tokens, up_cols, preferred_element_type=jnp.float32) * up_scale
    hidden = lax.optimization_barrier(jnp.square(jax.nn.relu(upper)).astype(jnp.bfloat16))
    partial = jnp.dot(hidden, down_part, preferred_element_type=jnp.float32).astype(jnp.bfloat16)
    total = scattered_sum(partial, n, rank, 5)
    return (middle.astype(jnp.float32) + total).astype(jnp.bfloat16)


def solution(mesh):
    in_specs = (
        P(("fs", "tp"), None),
        P(),
        P("fs", "tp"),
        P("fs", "tp"),
        P(),
        P(),
        P(),
        P(),
        P("tp", "fs"),
        P("fs"),
        P(),
        P("fs", "tp"),
        P("tp"),
        P("tp", "fs"),
        P("fs"),
    )
    out_specs = P(("fs", "tp"), None)
    return jax.shard_map(shards, mesh=mesh, in_specs=in_specs, out_specs=out_specs, check_vma=False)
```

```python
import functools

import jax
import jax.numpy as jnp
from jax import lax
from jax.experimental import pallas as pl
from jax.experimental.pallas import tpu as pltpu
from jax.sharding import PartitionSpec as P


GROUPS = 4
CORES = 2
MESH = pl.DeviceIdType.MESH


def rms_scaled(values, gain):
    data = values.astype(jnp.float32)
    return data * lax.rsqrt(jnp.mean(data * data, axis=-1, keepdims=True) + 1e-06) * gain


def depthwise(padded, taps, length):
    wide = padded.astype(jnp.float32)
    conv = jnp.zeros((length, wide.shape[1]), jnp.float32)
    for offset in range(taps.shape[0]):
        conv = conv + taps[offset] * wide[offset : offset + length]
    return conv


def place(n):
    me = lax.axis_index("tp")
    core = lax.rem(me, CORES)
    chip = me // CORES
    chips = n // CORES
    partner = chip * CORES + (CORES - 1 - core)
    return me, core, chip, chips, partner


def chip_core(chip, core, chips):
    return lax.rem(chip + 2 * chips, chips) * CORES + core


def greet(core, chip, chips, partner):
    barrier = pltpu.get_barrier_semaphore()
    pl.semaphore_signal(barrier, inc=1, device_id={"tp": partner}, device_id_type=MESH)
    for d in range(1, chips):
        pl.semaphore_signal(
            barrier, inc=1, device_id={"tp": chip_core(chip + d, core, chips)}, device_id_type=MESH
        )
    pl.semaphore_wait(barrier, chips)


def gather_kernel(n, pieces, x_ref, out_ref, own_sem, far_send, far_recv, near_send, near_recv):
    me, core, chip, chips, partner = place(n)
    rows = x_ref.shape[0]
    step = rows // pieces
    greet(core, chip, chips, partner)

    def spot(owner, k):
        return out_ref.at[pl.ds(pl.multiple_of(owner * rows + k * step, step), step)]

    def src(k):
        return x_ref.at[pl.ds(k * step, step)]

    def far(d, k, owner, target):
        return pltpu.make_async_remote_copy(
            src_ref=src(k), dst_ref=spot(owner, k), send_sem=far_send.at[d - 1, k],
            recv_sem=far_recv.at[d - 1, k], device_id={"tp": target}, device_id_type=MESH)

    def near(d, k, owner, own):
        return pltpu.make_async_remote_copy(
            src_ref=src(k) if own else spot(owner, k), dst_ref=spot(owner, k),
            send_sem=near_send.at[d, k], recv_sem=near_recv.at[d, k],
            device_id={"tp": partner}, device_id_type=MESH)

    for k in range(pieces):
        for d in range(1, chips):
            far(d, k, me, chip_core(chip + d, core, chips)).start()
    for k in range(pieces):
        near(0, k, me, True).start()
    own = pltpu.make_async_copy(x_ref, out_ref.at[pl.ds(pl.multiple_of(me * rows, rows), rows)], own_sem)
    own.start()
    for k in range(pieces):
        for d in range(1, chips):
            owner = chip_core(chip - d, core, chips)
            far(d, k, owner, partner).wait_recv()
            near(d, k, owner, False).start()
    own.wait()
    for k in range(pieces):
        for d in range(1, chips):
            far(d, k, me, chip_core(chip + d, core, chips)).wait_send()
        for d in range(chips):
            sent = chip_core(chip - d, core, chips)
            got = chip_core(chip - d, CORES - 1 - core, chips)
            near(d, k, sent, d == 0).wait_send()
            near(d, k, got, d == 0).wait_recv()


def tp_gather(x, n, cid):
    rows, width = x.shape
    chips = n // CORES
    pieces = 4
    sent = 2 * rows * width * (n - 1)
    return pl.pallas_call(
        functools.partial(gather_kernel, n, pieces),
        out_shape=jax.ShapeDtypeStruct((rows * n, width), x.dtype),
        in_specs=[pl.BlockSpec(memory_space=pltpu.VMEM)],
        out_specs=pl.BlockSpec(memory_space=pl.ANY),
        scratch_shapes=[
            pltpu.SemaphoreType.DMA,
            pltpu.SemaphoreType.DMA((chips - 1, pieces)),
            pltpu.SemaphoreType.DMA((chips - 1, pieces)),
            pltpu.SemaphoreType.DMA((chips, pieces)),
            pltpu.SemaphoreType.DMA((chips, pieces)),
        ],
        compiler_params=pltpu.CompilerParams(collective_id=cid, has_side_effects=True),
        cost_estimate=pl.CostEstimate(flops=200_000_000, bytes_accessed=sent, transcendentals=0),
        name="tp_gather",
    )(x)


def scatter_kernel(n, pieces, p_ref, near_ref, far_ref, mine, theirs, load_sem, near_send, near_recv, far_send, far_recv):
    _, core, chip, chips, partner = place(n)
    rows = near_ref.shape[0]
    step = rows // pieces
    other = CORES - 1 - core
    greet(core, chip, chips, partner)

    def part(owner, k):
        return p_ref.at[pl.ds(pl.multiple_of(owner * rows + k * step, step), step)]

    def near(d, k):
        dst = near_ref.at[pl.ds(k * step, step)] if d == 0 else theirs.at[d - 1, pl.ds(k * step, step)]
        return pltpu.make_async_remote_copy(
            src_ref=part(chip_core(chip + d, other, chips), k), dst_ref=dst,
            send_sem=near_send.at[d, k], recv_sem=near_recv.at[d, k],
            device_id={"tp": partner}, device_id_type=MESH)

    def load(d, k):
        return pltpu.make_async_copy(
            part(chip_core(chip + d, core, chips), k), mine.at[d - 1, pl.ds(k * step, step)], load_sem.at[d - 1, k])

    def far(d, k):
        return pltpu.make_async_remote_copy(
            src_ref=mine.at[d - 1, pl.ds(k * step, step)], dst_ref=far_ref.at[d - 1, pl.ds(k * step, step)],
            send_sem=far_send.at[d - 1, k], recv_sem=far_recv.at[d - 1, k],
            device_id={"tp": chip_core(chip + d, core, chips)}, device_id_type=MESH)

    for k in range(pieces):
        for d in range(1, chips):
            near(d, k).start()
            load(d, k).start()
    for k in range(pieces):
        near(0, k).start()
    for k in range(pieces):
        for d in range(1, chips):
            near(d, k).wait_recv()
            load(d, k).wait()
            at = pl.ds(k * step, step)
            total = mine[d - 1, at].astype(jnp.float32) + theirs[d - 1, at].astype(jnp.float32)
            mine[d - 1, at] = total.astype(mine.dtype)
            far(d, k).start()
    for k in range(pieces):
        near(0, k).wait_recv()
        for d in range(chips):
            near(d, k).wait_send()
        for d in range(1, chips):
            far(d, k).wait()


def tp_scatter(part, n, cid):
    rows, width = part.shape[0] // n, part.shape[1]
    chips = n // CORES
    pieces = 4
    sent = 2 * rows * width * (n - 1)
    return pl.pallas_call(
        functools.partial(scatter_kernel, n, pieces),
        out_shape=(
            jax.ShapeDtypeStruct((rows, width), part.dtype),
            jax.ShapeDtypeStruct((chips - 1, rows, width), part.dtype),
        ),
        in_specs=[pl.BlockSpec(memory_space=pl.ANY)],
        out_specs=(pl.BlockSpec(memory_space=pl.ANY), pl.BlockSpec(memory_space=pl.ANY)),
        scratch_shapes=[
            pltpu.VMEM((chips - 1, rows, width), part.dtype),
            pltpu.VMEM((chips - 1, rows, width), part.dtype),
            pltpu.SemaphoreType.DMA((chips - 1, pieces)),
            pltpu.SemaphoreType.DMA((chips, pieces)),
            pltpu.SemaphoreType.DMA((chips, pieces)),
            pltpu.SemaphoreType.DMA((chips - 1, pieces)),
            pltpu.SemaphoreType.DMA((chips - 1, pieces)),
        ],
        compiler_params=pltpu.CompilerParams(collective_id=cid, has_side_effects=True),
        cost_estimate=pl.CostEstimate(flops=200_000_000, bytes_accessed=sent, transcendentals=0),
        name="tp_scatter",
    )(part)


def scattered_sum(part, n, rank, cid):
    rows = part.shape[0] // n
    near, far = tp_scatter(part, n, cid)
    own = lax.dynamic_slice_in_dim(part, rank * rows, rows, 0)
    total = own.astype(jnp.float32) + near.astype(jnp.float32)
    for d in range(far.shape[0]):
        total = total + far[d].astype(jnp.float32)
    return total


def stats_kernel(n, x_ref, out_ref, recv, send_sem, recv_sem):
    me = lax.axis_index("tp")
    barrier = pltpu.get_barrier_semaphore()
    for d in range(1, n):
        pl.semaphore_signal(barrier, inc=1, device_id={"tp": lax.rem(me + d, n)}, device_id_type=MESH)
    pl.semaphore_wait(barrier, n - 1)

    def send(d):
        return pltpu.make_async_remote_copy(
            src_ref=x_ref, dst_ref=recv.at[d - 1], send_sem=send_sem.at[d - 1],
            recv_sem=recv_sem.at[d - 1], device_id={"tp": lax.rem(me + d, n)}, device_id_type=MESH)

    for d in range(1, n):
        send(d).start()
    total = x_ref[...]
    for d in range(1, n):
        send(d).wait_recv()
        total = total + recv[d - 1]
    out_ref[...] = total
    for d in range(1, n):
        send(d).wait_send()


def tp_sum(x, n, cid):
    return pl.pallas_call(
        functools.partial(stats_kernel, n),
        out_shape=jax.ShapeDtypeStruct(x.shape, x.dtype),
        in_specs=[pl.BlockSpec(memory_space=pltpu.VMEM)],
        out_specs=pl.BlockSpec(memory_space=pltpu.VMEM),
        scratch_shapes=[
            pltpu.VMEM((n - 1,) + x.shape, x.dtype),
            pltpu.SemaphoreType.DMA((n - 1,)),
            pltpu.SemaphoreType.DMA((n - 1,)),
        ],
        compiler_params=pltpu.CompilerParams(collective_id=cid, has_side_effects=True),
        cost_estimate=pl.CostEstimate(flops=20_000_000, bytes_accessed=4 * x.size * n, transcendentals=0),
        name="tp_sum",
    )(x)


def ring_at(q, count):
    q = lax.rem(q + 2 * count, count)
    high = q // (count // 2)
    return (1 - high) * 2 * q + high * (2 * (count - 1 - q) + 1)


def mlp_kernel(
    n, count, tok_ref, up_ref, scale_ref, w_ref, mid_ref, out_ref,
    hidden, held, part, theirs, near_in, far_in,
    cw_send, cw_recv, ccw_send, ccw_recv, near_send, near_recv, far_send, far_recv,
):
    me, core, chip, chips, partner = place(n)
    seat = lax.axis_index("fs")
    odd = lax.rem(seat, 2)
    pos = (1 - odd) * (seat // 2) + odd * (count - 1 - seat // 2)
    right, left = ring_at(pos + 1, count), ring_at(pos - 1, count)
    rows, width = mid_ref.shape[0], w_ref.shape[1]
    depth = w_ref.shape[0]
    half = depth // 2
    far_step = count // 2
    other = CORES - 1 - core
    tile = 256

    barrier = pltpu.get_barrier_semaphore()
    for target in (left, right):
        pl.semaphore_signal(barrier, inc=1, device_id={"fs": target}, device_id_type=MESH)
    pl.semaphore_signal(barrier, inc=1, device_id={"tp": partner}, device_id_type=MESH)
    for d in range(1, chips):
        pl.semaphore_signal(
            barrier, inc=1, device_id={"tp": chip_core(chip + d, core, chips)}, device_id_type=MESH
        )
    pl.semaphore_wait(barrier, chips + 2)

    def hop(s, k, clockwise):
        at = pl.ds(k * half, half)
        before = s - 1 if clockwise else count - s + 1
        after = s if clockwise else count - s
        src = w_ref.at[at] if s == 1 else held.at[before, at]
        return pltpu.make_async_remote_copy(
            src_ref=src, dst_ref=held.at[after, at],
            send_sem=(cw_send if clockwise else ccw_send).at[s - 1, k],
            recv_sem=(cw_recv if clockwise else ccw_recv).at[s - 1, k],
            device_id={"fs": right if clockwise else left}, device_id_type=MESH)

    def carries(s, k, clockwise):
        return s < far_step or (s == far_step and k == (0 if clockwise else 1))

    def pass_on(s, k):
        for clockwise in (True, False):
            if carries(s, k, clockwise):
                hop(s, k, clockwise).wait_recv()
                if carries(s + 1, k, clockwise):
                    hop(s + 1, k, clockwise).start()

    def expand(piece, pieces):
        span = up_ref.shape[1] // pieces
        block = min(512, span)

        @pl.loop(0, tok_ref.shape[0] // tile)
        def _(t):
            at = pl.ds(pl.multiple_of(t * tile, tile), tile)
            for c in range(piece * span, (piece + 1) * span, block):
                upper = jnp.dot(tok_ref[at, :], up_ref[:, c : c + block], preferred_element_type=jnp.float32)
                upper = jnp.maximum(upper * scale_ref[:, c : c + block], 0.0)
                hidden[at, c : c + block] = (upper * upper).astype(hidden.dtype)

    def rows_of(owner):
        return pl.ds(pl.multiple_of(owner * rows, rows), rows)

    def near(j, d):
        return pltpu.make_async_remote_copy(
            src_ref=part.at[j, rows_of(chip_core(chip + d, other, chips))],
            dst_ref=near_in.at[j] if d == 0 else theirs.at[j, d - 1],
            send_sem=near_send.at[j, d], recv_sem=near_recv.at[j, d],
            device_id={"tp": partner}, device_id_type=MESH)

    def far(j, d):
        return pltpu.make_async_remote_copy(
            src_ref=part.at[j, rows_of(chip_core(chip + d, core, chips))], dst_ref=far_in.at[j, d - 1],
            send_sem=far_send.at[j, d - 1], recv_sem=far_recv.at[j, d - 1],
            device_id={"tp": chip_core(chip + d, core, chips)}, device_id_type=MESH)

    def contract(j):
        @pl.loop(0, tok_ref.shape[0] // tile)
        def _(t):
            at = pl.ds(pl.multiple_of(t * tile, tile), tile)
            weight = w_ref[...] if j == 0 else held[j]
            part[j, at, :] = jnp.dot(hidden[at, :], weight, preferred_element_type=jnp.float32).astype(part.dtype)

        for d in list(range(1, chips)) + [0]:
            near(j, d).start()

    def combine(j):
        for d in range(1, chips):
            near(j, d).wait_recv()
            at = rows_of(chip_core(chip + d, core, chips))
            total = part[j, at, :].astype(jnp.float32) + theirs[j, d - 1].astype(jnp.float32)
            part[j, at, :] = total.astype(part.dtype)
            far(j, d).start()

    def finish(j):
        near(j, 0).wait_recv()
        total = part[j, rows_of(me), :].astype(jnp.float32) + near_in[j].astype(jnp.float32)
        for d in range(1, chips):
            far(j, d).wait_recv()
            total = total + far_in[j, d - 1].astype(jnp.float32)
        at = pl.ds(pl.multiple_of(ring_at(pos - j, count) * width, width), width)
        out_ref[:, at] = (mid_ref[:, at].astype(jnp.float32) + total).astype(out_ref.dtype)

    for k in range(2):
        for clockwise in (True, False):
            if carries(1, k, clockwise):
                hop(1, k, clockwise).start()
    expand(0, 2)
    pass_on(1, 0)
    expand(1, 2)
    pass_on(1, 1)
    groups = [[0]] + [[s, count - s] if s < far_step else [s] for s in range(1, far_step + 1)]
    for s, group in enumerate(groups):
        if s > 1:
            pass_on(s, 0)
            pass_on(s, 1)
        for j in group:
            contract(j)
        for j in group:
            combine(j)
        if s > 1:
            for j in groups[s - 2]:
                finish(j)
    for group in groups[-2:]:
        for j in group:
            finish(j)
    for s in range(1, far_step + 1):
        for k in range(2):
            for clockwise in (True, False):
                if carries(s, k, clockwise):
                    hop(s, k, clockwise).wait_send()
    for j in range(count):
        for d in range(chips):
            near(j, d).wait_send()
        for d in range(1, chips):
            far(j, d).wait_send()


def ring_mlp(tokens, up_cols, up_scale, down, middle, n, count, cid):
    seq, rows = tokens.shape[0], middle.shape[0]
    depth, width = down.shape
    chips = n // CORES
    kind = tokens.dtype
    steps = count // 2
    dma = pltpu.SemaphoreType.DMA
    return pl.pallas_call(
        functools.partial(mlp_kernel, n, count),
        out_shape=jax.ShapeDtypeStruct(middle.shape, middle.dtype),
        in_specs=[pl.BlockSpec(memory_space=pltpu.VMEM)] * 5,
        out_specs=pl.BlockSpec(memory_space=pltpu.VMEM),
        scratch_shapes=[
            pltpu.VMEM((seq, depth), kind),
            pltpu.VMEM((count, depth, width), kind),
            pltpu.VMEM((count, seq, width), kind),
            pltpu.VMEM((count, chips - 1, rows, width), kind),
            pltpu.VMEM((count, rows, width), kind),
            pltpu.VMEM((count, chips - 1, rows, width), kind),
            dma((steps, 2)), dma((steps, 2)), dma((steps, 2)), dma((steps, 2)),
            dma((count, chips)), dma((count, chips)), dma((count, chips - 1)), dma((count, chips - 1)),
        ],
        compiler_params=pltpu.CompilerParams(
            collective_id=cid, has_side_effects=True, vmem_limit_bytes=60 * 1024 * 1024
        ),
        cost_estimate=pl.CostEstimate(flops=4 * seq * depth * width * count, bytes_accessed=4 * seq * depth, transcendentals=0),
        name="ring_mlp",
    )(tokens, up_cols, up_scale.reshape(1, -1), down, middle)


def shards(
    resid,
    norm1_gain,
    w_value,
    w_gate,
    value_scale,
    gate_scale,
    conv_taps,
    conv_gain,
    w_point,
    point_scale,
    norm2_gain,
    w_up,
    up_scale,
    w_down,
    down_scale,
):
    tok_rows = resid.shape[0]
    n = lax.axis_size("tp")
    rank = lax.axis_index("tp")
    seq_len = tok_rows * n
    channels = value_scale.shape[0]
    group_width = channels // GROUPS
    reach = conv_taps.shape[0] // 2
    own_width = w_value.shape[1]
    first_bf = jnp.concatenate(
        [w_value.astype(jnp.bfloat16), w_gate.astype(jnp.bfloat16), (w_point * point_scale).T.astype(jnp.bfloat16)],
        axis=1,
    )
    first_rows = lax.all_gather(first_bf, "fs", axis=0, tiled=True)
    up_cols = lax.all_gather(w_up.astype(jnp.bfloat16), "fs", axis=0, tiled=True)
    down_bf = (w_down * down_scale).astype(jnp.bfloat16)
    first = rank * own_width
    own_value_scale = lax.dynamic_slice_in_dim(value_scale, first, own_width, 0)
    own_gate_scale = lax.dynamic_slice_in_dim(gate_scale, first, own_width, 0)
    own_taps = lax.dynamic_slice_in_dim(conv_taps, first, own_width, 1)
    own_gain = lax.dynamic_slice_in_dim(conv_gain, first, own_width, 0)
    normed = rms_scaled(resid, norm1_gain).astype(jnp.bfloat16)
    piece = tp_gather(normed, n, 1)
    value = jnp.dot(piece, first_rows[:, :own_width], preferred_element_type=jnp.float32) * own_value_scale
    gate = (
        jnp.dot(piece, first_rows[:, own_width : 2 * own_width], preferred_element_type=jnp.float32)
        * own_gate_scale
    )
    glu_seq = (value * jax.nn.sigmoid(gate)).astype(jnp.bfloat16)
    padded = jnp.pad(glu_seq, ((reach, reach), (0, 0)))
    conv = depthwise(padded, own_taps, seq_len)
    member = ((first + jnp.arange(own_width)) % GROUPS)[None, :] == jnp.arange(GROUPS)[:, None]
    member = member.astype(jnp.float32)
    flip = (((1,), (1,)), ((), ()))
    sums = lax.dot_general(member, conv, flip, precision=lax.Precision.HIGHEST)
    squares = lax.dot_general(member, conv * conv, flip, precision=lax.Precision.HIGHEST)
    totals = tp_sum(jnp.concatenate([sums, squares], axis=0), n, 2)
    spread = (((0,), (0,)), ((), ()))
    gmean = lax.dot_general(totals[:GROUPS] / group_width, member, spread, precision=lax.Precision.HIGHEST)
    gsquare = lax.dot_general(totals[GROUPS:] / group_width, member, spread, precision=lax.Precision.HIGHEST)
    scaled = (conv - gmean) * lax.rsqrt(gsquare - gmean * gmean + 1e-05) * own_gain
    act = jax.nn.silu(scaled).astype(jnp.bfloat16)
    mixed_part = lax.dot_general(
        act, first_rows[:, 2 * own_width :], flip, preferred_element_type=jnp.float32
    ).astype(jnp.bfloat16)
    mixed = scattered_sum(mixed_part, n, rank, 3)
    middle = (resid.astype(jnp.float32) + mixed).astype(jnp.bfloat16)
    normed2 = rms_scaled(middle, norm2_gain).astype(jnp.bfloat16)
    tokens = tp_gather(normed2, n, 4)
    return ring_mlp(tokens, up_cols, up_scale, down_bf, middle, n, lax.axis_size("fs"), 5)


def solution(mesh):
    in_specs = (
        P(("fs", "tp"), None),
        P(),
        P("fs", "tp"),
        P("fs", "tp"),
        P(),
        P(),
        P(),
        P(),
        P("tp", "fs"),
        P("fs"),
        P(),
        P("fs", "tp"),
        P("tp"),
        P("tp", "fs"),
        P("fs"),
    )
    out_specs = P(("fs", "tp"), None)
    return jax.shard_map(shards, mesh=mesh, in_specs=in_specs, out_specs=out_specs, check_vma=False)
```
